32 devices in a mesh: ra: 8 (over z, x), cb: 4 (over y, core).
Axes of the slice: x: 2, y: 2, z: 4, core: 2. Of those that a mesh axis runs over, the one named last changes fastest.
Arguments:
- tokens: bfloat16 [384, 4096], P(None, 'ra'), may hold values from -260 to 260
- up_weight: float32 [2, 4096, 16384], P(None, 'ra', 'cb'), may hold values from -0.125 to 0.125
- up_scale: float32 [2, 16384], P(None, 'cb'), may hold values from 0.5 to 2
- down_weight: float32 [2, 16384, 4096], P(None, 'cb', 'ra'), may hold values from -0.046875 to 0.046875
- down_scale: float32 [2, 4096], P(None, 'ra'), may hold values from 0.7 to 14
- pre_gain: float32 [2, 4096], P(None, 'ra'), may hold values from 0.1 to 1.9
- post_gain: float32 [2, 4096], P(None, 'ra'), may hold values from 0.1 to 1.9
Outputs:
- stream_out: bfloat16 [384, 4096], P(None, 'ra')
The draws below stay inside these ranges and needn't reach their ends.
All inputs are finite; a program needn't handle non-finite values.
Results may differ from the reference program's by a relative error of at most 0.023.
Values may be sent and summed in bfloat16 or wider, within the bound.
A program may use at most 128 MiB of HBM per device.

```python
import math
import jax
import jax.numpy as jnp
from jax import lax

D = 4096
FF = 16384
LAYERS = 2
TOKENS = 384
N_CB = 4


def draw_tokens(key, part):
    first = jax.random.fold_in(key, 11)
    second = jax.random.fold_in(key, 12)
    third = jax.random.fold_in(key, 13)
    column_scale = 10.0 ** (jnp.arange(D, dtype=jnp.float32) / D) * jax.random.uniform(second, (D,), jnp.float32, 0.7, 1.4)
    row_scale = 10.0 ** jax.random.uniform(third, (TOKENS, 1), jnp.float32)
    base = jnp.clip(jax.random.normal(first, (TOKENS, D), jnp.float32), -6.0, 6.0)
    return (0.3 * base * row_scale * column_scale[None, :]).astype(jnp.bfloat16)


def draw_down_scale(key, part):
    first = jax.random.fold_in(key, 21)
    rising = 10.0 ** (jnp.arange(D, dtype=jnp.float32) / D)
    rough = jnp.exp(jax.random.uniform(first, (LAYERS, D), jnp.float32, jnp.log(0.7), jnp.log(1.4)))
    return (rough * rising[None, :]).astype(jnp.float32)


def strengthened(entries, rng, source, target, parts, factor):
    def block_of(dim):
        return (jnp.arange(entries.shape[dim]) // (entries.shape[dim] // parts)).reshape((-1,) + (1,) * (entries.ndim - 1 - dim))

    one_side = jax.random.permutation(rng, parts)[block_of(target)]
    second = (block_of(target) + parts // 2) % parts
    return jnp.where((block_of(source) == one_side) | (block_of(source) == second), factor * entries, entries)


def block_scale(stream_key, dims, shards, smallest, largest):
    def one(dim, shards_of):
        draws = jax.random.uniform(jax.random.fold_in(jax.random.fold_in(stream_key, 6), dim), (shards_of,), jnp.float32, smallest / len(shards), largest / len(shards))
        return jnp.repeat(jnp.exp(draws), dims[dim] // shards_of).reshape((-1,) + (1,) * (len(dims) - dim - 1))

    factor_of = one(*shards[0])
    for cut in shards[1:]:
        factor_of = factor_of * one(*cut)
    return factor_of


def gaussian(key, dims, width, bound, pieces=(), held_as=jnp.bfloat16):
    loudness = block_scale(key, dims, pieces, -0.22, 0.18) if pieces else 1.0
    values = jax.random.normal(key, dims, jnp.float32) * width * loudness
    return jnp.minimum(jnp.maximum(values, -bound), bound).astype(held_as)


def heavy_noise(own_key, extent, deviation, limit, split, heavy, held_as=jnp.bfloat16):
    drawn = deviation * jax.random.normal(own_key, extent, jnp.float32)
    if split:
        drawn = drawn * block_scale(own_key, extent, split, -0.22, 0.18)
    return jnp.clip(strengthened(drawn, jax.random.fold_in(own_key, 3), *heavy), -limit, limit).astype(held_as)


def setup_inputs(seed: int = 0) -> dict:
    key_of = jax.random.split(jax.random.key(seed), 8)
    return {
        "tokens": draw_tokens(jax.random.fold_in(key_of[7], 71), 0),
        "up_weight": heavy_noise(key_of[1], (LAYERS, D, FF), D ** -0.5, 0.125, ((1, 8), (2, 4)), (1, 2, 8, 2.0), jnp.float32),
        "up_scale": jnp.clip(jnp.exp(math.log(2.0) - 1.3862944 * jax.random.uniform(key_of[2], (LAYERS, FF), jnp.float32) ** block_scale(key_of[2], (LAYERS, FF), ((1, 4),), -0.2, 0.2)), 0.5, 2.0),
        "down_weight": gaussian(key_of[3], (LAYERS, FF, D), FF ** -0.5, 0.046875, ((1, 4), (2, 8)), jnp.float32),
        "down_scale": draw_down_scale(jax.random.fold_in(key_of[7], 71), 0),
        "pre_gain": jnp.clip(1.0 + 0.18 * jax.random.normal(key_of[5], (LAYERS, D), jnp.float32), 0.1, 1.9),
        "post_gain": jnp.clip(1.0 + 0.18 * jax.random.normal(key_of[6], (LAYERS, D), jnp.float32), 0.1, 1.9),
    }


norm_eps = 1e-06
residual_keep = 0.5

def reference(tokens, up_weight, up_scale, down_weight, down_scale, pre_gain, post_gain):
    stream = tokens
    for sublayer in range(LAYERS):
        values = stream.astype(jnp.float32)
        scaled = (values * pre_gain[sublayer][None, :]).astype(jnp.bfloat16)
        whole_up = jnp.dot(scaled, up_weight[sublayer].astype(jnp.bfloat16), preferred_element_type=jnp.float32)
        whole_up = whole_up * up_scale[sublayer][None, :]
        hidden = jnp.square(jax.nn.relu(whole_up)).astype(jnp.bfloat16)
        block_hidden = hidden.reshape(TOKENS, N_CB, FF // N_CB).astype(jnp.float32)
        block_down = down_weight[sublayer].astype(jnp.bfloat16).reshape(N_CB, FF // N_CB, D).astype(jnp.float32)
        partials = jnp.einsum('mbf,bfd->bmd', block_hidden, block_down).astype(jnp.bfloat16)
        partials = lax.optimization_barrier(partials).astype(jnp.float32)
        branch_in = lax.optimization_barrier(jnp.sum(partials, axis=0)) * down_scale[sublayer][None, :]
        inv_post = lax.rsqrt(lax.optimization_barrier(jnp.mean(branch_in * branch_in, axis=1, keepdims=True)) + norm_eps)
        branch = branch_in * inv_post * post_gain[sublayer][None, :]
        stream = (residual_keep * values + branch).astype(jnp.bfloat16)
    return stream
```

```python
import functools

import jax
import jax.numpy as jnp
from jax import lax
from jax.experimental import pallas as pl
from jax.experimental.pallas import tpu as pltpu
from jax.sharding import PartitionSpec as P

norm_eps = 1e-06
residual_keep = 0.5
MESH = pl.DeviceIdType.MESH
STREAMS = 2
PIECES = 2
TAIL_IN_SCATTER = (1, 1, 2, 4, 5, 6)
TAIL_IN_GATHER = (0, 0, 1, 3, 4, 5)
LANES = 128
BF16_ROWS = 16


def plain(tokens, up_weight, up_scale, down_weight, down_scale, pre_gain, post_gain):
    values = tokens.astype(jnp.float32)
    model_width = tokens.shape[1] * lax.axis_size("ra")
    stream = tokens
    for sublayer in range(up_weight.shape[0]):
        scaled = (values * pre_gain[sublayer][None, :]).astype(jnp.bfloat16)
        up_matrix = up_weight[sublayer].astype(jnp.bfloat16)
        down_matrix = down_weight[sublayer].astype(jnp.bfloat16)
        partial_up = jnp.dot(scaled, up_matrix, preferred_element_type=jnp.float32)
        whole_up = lax.psum(partial_up.astype(jnp.bfloat16), "ra").astype(jnp.float32)
        hidden = jnp.square(jax.nn.relu(whole_up * up_scale[sublayer][None, :])).astype(
            jnp.bfloat16
        )
        partial_down = jnp.dot(hidden, down_matrix, preferred_element_type=jnp.float32)
        summed = lax.psum(partial_down.astype(jnp.bfloat16), "cb").astype(jnp.float32)
        branch_in = summed * down_scale[sublayer][None, :]
        post_squares = lax.psum(jnp.sum(branch_in * branch_in, axis=1), "ra")
        inv_post = lax.rsqrt(post_squares / model_width + norm_eps)[:, None]
        branch = branch_in * inv_post * post_gain[sublayer][None, :]
        stream = (residual_keep * values + branch).astype(jnp.bfloat16)
        values = stream.astype(jnp.float32)
    return stream


def kernel(
    n, m, layers,
    tok, up, us, dn, ds, pg, qg,
    out,
    st_up, st_dn, wu, wd, xs, own, sendb, recvb, hid, acc, core_s, core_r, pair, bbuf, ssq, ssall,
    w_sem, rs_s, rs_r, ag_s, ag_r, co_s, co_r, pr_s, pr_r, bs_s, bs_r, ss_s, ss_r,
):
    f32, bf16 = jnp.float32, jnp.bfloat16
    ra, cb = lax.axis_index("ra"), lax.axis_index("cb")
    rows = xs.shape[1]
    dl = tok.shape[1]
    fc = wu.shape[2]
    fh = fc // 2
    sub = rows // PIECES
    far = n // 2
    core, pairs = lax.rem(cb, 2), m // 2
    lane_rows = ssq.shape[0]

    def wrap(i):
        return lax.rem(i + 2 * n, n)

    half, odd = lax.div(ra, 2), lax.rem(ra, 2)
    p = half + odd * (n - 1 - 2 * half)

    def ra_of(q):
        hi = lax.div(q, n // 2)
        return 2 * q * (1 - hi) + hi * (2 * (n - 1 - q) + 1)

    target = [ra_of(wrap(p + 1)), ra_of(wrap(p - 1))]
    sign = [1, -1]
    long_flows = [(0, 0), (1, 1)]
    short_flows = [(0, 1), (1, 0)]
    flows = long_flows + short_flows

    def hops(d, e):
        return far if d == e else far - 1

    def chunk(q):
        return wrap(p + q)

    near_first = [0] + [q for k in range(1, far) for q in (k, -k)] + [far]
    far_first = near_first[::-1]

    def up_copy(l, i):
        c = chunk(far_first[i])
        return pltpu.make_async_copy(
            up.at[l, :, pl.ds(pl.multiple_of(c * fc, fc), fc)], st_up.at[i], w_sem.at[0, i]
        )

    def dn_copy(l, i):
        c = chunk(near_first[i])
        return pltpu.make_async_copy(
            dn.at[l, pl.ds(pl.multiple_of(c * fc, fc), fc), :], st_dn.at[i], w_sem.at[1, i]
        )

    def convert(src, dst, i, c):
        block = 32

        def body(j, _):
            r = pl.ds(pl.multiple_of(j * block, block), block)
            dst[c, r, :] = src[i, r, :].astype(bf16)
            return 0

        lax.fori_loop(0, src.shape[1] // block, body, 0)

    def take_up(l, chosen):
        for i in chosen:
            up_copy(l, i).wait()
            convert(st_up, wu, i, chunk(far_first[i]))
            if l + 1 < layers:
                up_copy(l + 1, i).start()

    def take_dn(l, chosen):
        for i in chosen:
            dn_copy(l, i).wait()
            convert(st_dn, wd, i, chunk(near_first[i]))
            if l + 1 < layers:
                dn_copy(l + 1, i).start()

    def part(h):
        return pl.ds(h * sub, sub)

    def rs_copy(l, g, d, e, j, h):
        return pltpu.make_async_remote_copy(
            src_ref=sendb.at[g, d, e, j, part(h), :],
            dst_ref=recvb.at[l, g, d, e, j, part(h), :],
            send_sem=rs_s.at[l, g, d, e, j, h], recv_sem=rs_r.at[l, g, d, e, j, h],
            device_id={"ra": target[d]}, device_id_type=MESH,
        )

    def ag_copy(l, g, d, e, s, h, arriving=False):
        c = chunk(-sign[d] * (s if arriving else s - 1))
        piece = hid.at[l, g, c, e, part(h), :]
        return pltpu.make_async_remote_copy(
            src_ref=piece, dst_ref=piece,
            send_sem=ag_s.at[l, g, d, e, s - 1, h], recv_sem=ag_r.at[l, g, d, e, s - 1, h],
            device_id={"ra": target[d]}, device_id_type=MESH,
        )

    def core_copy(l, g):
        return pltpu.make_async_remote_copy(
            src_ref=core_s.at[l, g], dst_ref=core_r.at[l, g],
            send_sem=co_s.at[l, g], recv_sem=co_r.at[l, g],
            device_id={"cb": cb + 1 - 2 * core}, device_id_type=MESH,
        )

    def pair_copy(l, g, k, who):
        return pltpu.make_async_remote_copy(
            src_ref=pair.at[l, g, who], dst_ref=pair.at[l, g, who],
            send_sem=pr_s.at[l, g, k - 1], recv_sem=pr_r.at[l, g, k - 1],
            device_id={"cb": lax.rem(cb + 2 * k, m)}, device_id_type=MESH,
        )

    def branch_copy(l, g, who):
        return pltpu.make_async_remote_copy(
            src_ref=bbuf.at[l, g, who], dst_ref=bbuf.at[l, g, who],
            send_sem=bs_s.at[l, g], recv_sem=bs_r.at[l, g],
            device_id={"cb": cb + 1 - 2 * core}, device_id_type=MESH,
        )

    def ss_copy(l, g, k, who):
        return pltpu.make_async_remote_copy(
            src_ref=ssall.at[l, g, who], dst_ref=ssall.at[l, g, who],
            send_sem=ss_s.at[l, g, k - 1], recv_sem=ss_r.at[l, g, k - 1],
            device_id={"ra": lax.rem(ra + k, n)}, device_id_type=MESH,
        )

    def dot(a, b):
        return jnp.dot(a, b, preferred_element_type=f32)

    def project(g, q):
        c = chunk(q)
        own[g, c] = dot(xs[g], wu[c])

    def mine(g, q, e, h):
        return own[g, chunk(q), h * sub : (h + 1) * sub, e * fh : (e + 1) * fh]

    def scatter(l, g, k, which):
        for h in range(PIECES):
            for d, e in which:
                j = k if d == e else k - 1
                v = mine(g, sign[d] * (far - k), e, h)
                if j > 0:
                    rs_copy(l, g, d, e, j - 1, h).wait_recv()
                    v = v + recvb[l, g, d, e, j - 1, part(h), :].astype(f32)
                sendb[g, d, e, j, part(h), :] = v.astype(bf16)
                rs_copy(l, g, d, e, j, h).start()

    def activate(l, g):
        project(g, 0)
        for e in (0, 1):
            scale = us[l : l + 1, pl.ds(pl.multiple_of(p * fc + e * fh, fh), fh)]
            for h in range(PIECES):
                v = mine(g, 0, e, h)
                for d in (0, 1):
                    j = hops(d, e) - 1
                    rs_copy(l, g, d, e, j, h).wait_recv()
                    v = v + recvb[l, g, d, e, j, part(h), :].astype(f32)
                v = jnp.maximum(v * scale, 0.0)
                hid[l, g, p, e, part(h), :] = (v * v).astype(bf16)

    def forward(l, g, s, which):
        for h in range(PIECES):
            for d, e in which:
                if s > 1:
                    ag_copy(l, g, d, e, s - 1, h, arriving=True).wait_recv()
                if s <= hops(d, e):
                    ag_copy(l, g, d, e, s, h).start()

    def reduce_hidden(l, g, q, first=False):
        c = chunk(q)
        a = dot(hid[l, g, c, 0], wd[c, :fh, :]) + dot(hid[l, g, c, 1], wd[c, fh:, :])
        if first:
            acc[g] = a
        else:
            acc[g] += a

    mid = rows // 2

    def share_cores(l, g):
        core_s[l, g] = acc[g, pl.ds(pl.multiple_of((1 - core) * mid, mid), mid), :].astype(bf16)
        core_copy(l, g).start()

    def share_pairs(l, g):
        y = lax.div(cb, 2)
        kept = acc[g, pl.ds(pl.multiple_of(core * mid, mid), mid), :].astype(bf16).astype(f32)
        core_copy(l, g).wait_recv()
        pair[l, g, y] = (kept + core_r[l, g].astype(f32)).astype(bf16)
        for k in range(1, pairs):
            pair_copy(l, g, k, y).start()

    def squares(l, g, who):
        b = bbuf[l, g, who]
        b = b * b
        t = b[:, :LANES]
        for j in range(1, dl // LANES):
            t = t + b[:, j * LANES : (j + 1) * LANES]
        ssq[pl.ds(pl.multiple_of(who * mid, mid), mid), :] = t

    def share_branch(l, g):
        y = lax.div(cb, 2)
        for k in range(1, pairs):
            pair_copy(l, g, k, lax.rem(y + pairs - k, pairs)).wait_recv()
        b = pair[l, g, 0].astype(f32)
        for k in range(1, pairs):
            b = b + pair[l, g, k].astype(f32)
        bbuf[l, g, core] = b * ds[l : l + 1, :]
        branch_copy(l, g, core).start()
        squares(l, g, core)

    def share_squares(l, g):
        branch_copy(l, g, 1 - core).wait_recv()
        squares(l, g, 1 - core)
        t = jnp.sum(jnp.transpose(ssq[...]), axis=0, keepdims=True)
        ssall[l, g, ra] = jnp.broadcast_to(t, (8, lane_rows))
        for k in range(1, n):
            ss_copy(l, g, k, ra).start()

    def renew(l, g):
        for k in range(1, n):
            ss_copy(l, g, k, lax.rem(ra + n - k, n)).wait_recv()
        t = ssall[l, g, 0]
        for k in range(1, n):
            t = t + ssall[l, g, k]
        t = lax.rsqrt(t / (dl * n) + norm_eps)
        ssq[...] = jnp.transpose(jnp.broadcast_to(t[0:1, :], (LANES, lane_rows)))
        before = tok if l == 0 else out
        for who in (0, 1):
            inv = ssq[who * mid : (who + 1) * mid, :]
            at = slice(g * rows + who * mid, g * rows + (who + 1) * mid)
            for j in range(dl // LANES):
                col = slice(j * LANES, (j + 1) * LANES)
                branch = bbuf[l, g, who, :, col] * inv * qg[l : l + 1, col]
                new = (residual_keep * before[at, col].astype(f32) + branch).astype(bf16)
                out[at, col] = new
                if l + 1 < layers:
                    xs[g, who * mid : (who + 1) * mid, col] = (
                        new.astype(f32) * pg[l + 1 : l + 2, col]
                    ).astype(bf16)

    def drain_scatter(l, g):
        for d, e in flows:
            for j in range(hops(d, e)):
                for h in range(PIECES):
                    rs_copy(l, g, d, e, j, h).wait_send()

    def drain_rest(l, g):
        for d, e in flows:
            for s in range(1, hops(d, e) + 1):
                for h in range(PIECES):
                    ag_copy(l, g, d, e, s, h).wait_send()
        core_copy(l, g).wait_send()
        for k in range(1, pairs):
            pair_copy(l, g, k, lax.div(cb, 2)).wait_send()
        branch_copy(l, g, core).wait_send()
        for k in range(1, n):
            ss_copy(l, g, k, ra).wait_send()

    for i in range(n):
        up_copy(0, i).start()

    barrier = pltpu.get_barrier_semaphore()
    for k in range(1, n):
        pl.semaphore_signal(
            barrier, inc=1, device_id={"ra": lax.rem(ra + k, n)}, device_id_type=MESH
        )
    for k in range(1, m):
        pl.semaphore_signal(
            barrier, inc=1, device_id={"cb": lax.rem(cb + k, m)}, device_id_type=MESH
        )

    for g in range(STREAMS):
        xs[g] = (tok[g * rows : (g + 1) * rows, :].astype(f32) * pg[0:1, :]).astype(bf16)
    ssq[...] = jnp.zeros_like(ssq)

    def tail_steps(l, g):
        def end():
            forward(l, g, far + 1, long_flows)
            reduce_hidden(l, g, far)
            share_cores(l, g)

        def short_end():
            forward(l, g, far, short_flows)
            reduce_hidden(l, g, far - 1)
            reduce_hidden(l, g, 1 - far)

        return [
            short_end, end, lambda: share_pairs(l, g), lambda: share_branch(l, g),
            lambda: share_squares(l, g), lambda: renew(l, g),
        ]

    def scatter_steps(l, g):
        fresh = l == 0 and g == 0

        def first():
            if fresh:
                take_up(l, [0])
            project(g, far)
            if fresh:
                pl.semaphore_wait(barrier, n + m - 2)
            scatter(l, g, 0, long_flows)

        def short(k):
            if fresh:
                take_up(l, [2 * k - 1, 2 * k])
                if k == 1:
                    for i in range(n):
                        dn_copy(l, i).start()
                if k == far - 1:
                    take_up(l, [n - 1])
            project(g, far - k)
            project(g, k - far)
            scatter(l, g, k, short_flows)

        steps = [first]
        for k in range(1, far):
            steps.append(functools.partial(short, k))
            steps.append(functools.partial(scatter, l, g, k, long_flows))
        return steps

    def gather_steps(l, g):
        def begin():
            forward(l, g, 1, flows)
            reduce_hidden(l, g, 0, first=True)

        def short(s):
            forward(l, g, s, short_flows)
            reduce_hidden(l, g, s - 1)
            reduce_hidden(l, g, 1 - s)

        steps = [begin]
        for s in range(2, far + 1):
            steps.append(functools.partial(forward, l, g, s, long_flows))
            if s < far:
                steps.append(functools.partial(short, s))
        return steps

    def run(steps, side, slots):
        slots = [min(at, len(steps) - 1) for at in slots]
        for i, step in enumerate(steps):
            step()
            for extra, at in zip(side, slots):
                if at == i:
                    extra()

    pending, first_half, second_half = [], range(n // 2), range(n // 2, n)
    for l in range(layers):
        run(scatter_steps(l, 0), pending, TAIL_IN_SCATTER)
        run(
            scatter_steps(l, 1),
            [
                lambda: activate(l, 0), lambda: take_dn(l, first_half),
                lambda: take_dn(l, second_half),
            ],
            (1, 2, 3),
        )
        side = [lambda: activate(l, 1), lambda: drain_scatter(l, 0)]
        if l + 1 < layers:
            side += [
                lambda: take_up(l + 1, first_half), lambda: take_up(l + 1, second_half)
            ]
        run(gather_steps(l, 0), side, (0, 4, 2, 3))
        run(
            gather_steps(l, 1), tail_steps(l, 0) + [lambda: drain_scatter(l, 1)],
            TAIL_IN_GATHER + (4,),
        )
        pending = tail_steps(l, 1)
    for step in pending:
        step()
    for l in range(layers):
        for g in range(STREAMS):
            drain_rest(l, g)


def local(n, m, tokens, up_weight, up_scale, down_weight, down_scale, pre_gain, post_gain):
    t, dl = tokens.shape
    layers, _, fl = up_weight.shape
    fits = (
        n % 2 == 0 and n >= 4 and m % 2 == 0 and t % (STREAMS * PIECES * BF16_ROWS) == 0
        and t % (STREAMS * 2 * BF16_ROWS) == 0 and fl % (2 * n * LANES) == 0
        and dl % LANES == 0
    )
    if not fits:
        return plain(
            tokens, up_weight, up_scale, down_weight, down_scale, pre_gain, post_gain
        )
    rows, fc, far = t // STREAMS, fl // n, n // 2
    lane_rows = -(-rows // LANES) * LANES
    f32, bf16 = jnp.float32, jnp.bfloat16
    vmem = pl.BlockSpec(memory_space=pltpu.VMEM)
    hbm = pl.BlockSpec(memory_space=pl.ANY)
    dma = pltpu.SemaphoreType.DMA
    return pl.pallas_call(
        functools.partial(kernel, n, m, layers),
        out_shape=jax.ShapeDtypeStruct((t, dl), bf16),
        in_specs=[vmem, hbm, vmem, hbm, vmem, vmem, vmem],
        out_specs=vmem,
        scratch_shapes=[
            pltpu.VMEM((n, dl, fc), f32),
            pltpu.VMEM((n, fc, dl), f32),
            pltpu.VMEM((n, dl, fc), bf16),
            pltpu.VMEM((n, fc, dl), bf16),
            pltpu.VMEM((STREAMS, rows, dl), bf16),
            pltpu.VMEM((STREAMS, n, rows, fc), f32),
            pltpu.VMEM((STREAMS, 2, 2, far, rows, fc // 2), bf16),
            pltpu.VMEM((layers, STREAMS, 2, 2, far, rows, fc // 2), bf16),
            pltpu.VMEM((layers, STREAMS, n, 2, rows, fc // 2), bf16),
            pltpu.VMEM((STREAMS, rows, dl), f32),
            pltpu.VMEM((layers, STREAMS, rows // 2, dl), bf16),
            pltpu.VMEM((layers, STREAMS, rows // 2, dl), bf16),
            pltpu.VMEM((layers, STREAMS, m // 2, rows // 2, dl), bf16),
            pltpu.VMEM((layers, STREAMS, 2, rows // 2, dl), f32),
            pltpu.VMEM((lane_rows, LANES), f32),
            pltpu.VMEM((layers, STREAMS, n, 8, lane_rows), f32),
            dma((2, n)),
            dma((layers, STREAMS, 2, 2, far, PIECES)),
            dma((layers, STREAMS, 2, 2, far, PIECES)),
            dma((layers, STREAMS, 2, 2, far, PIECES)),
            dma((layers, STREAMS, 2, 2, far, PIECES)),
            dma((layers, STREAMS)),
            dma((layers, STREAMS)),
            dma((layers, STREAMS, max(m // 2 - 1, 1))),
            dma((layers, STREAMS, max(m // 2 - 1, 1))),
            dma((layers, STREAMS)),
            dma((layers, STREAMS)),
            dma((layers, STREAMS, n - 1)),
            dma((layers, STREAMS, n - 1)),
        ],
        compiler_params=pltpu.CompilerParams(
            collective_id=0, has_side_effects=True, vmem_limit_bytes=60 * 1024 * 1024
        ),
    )(tokens, up_weight, up_scale, down_weight, down_scale, pre_gain, post_gain)


def solution(mesh):
    return jax.shard_map(
        functools.partial(local, mesh.shape["ra"], mesh.shape["cb"]),
        mesh=mesh,
        in_specs=(
            P(None, "ra"),
            P(None, "ra", "cb"),
            P(None, "cb"),
            P(None, "cb", "ra"),
            P(None, "ra"),
            P(None, "ra"),
            P(None, "ra"),
        ),
        out_specs=P(None, "ra"),
        check_vma=False,
    )
```

```python
import functools

import jax
import jax.numpy as jnp
from jax import lax
from jax.experimental import pallas as pl
from jax.experimental.pallas import tpu as pltpu
from jax.sharding import PartitionSpec as P

norm_eps = 1e-06
residual_keep = 0.5
MESH = pl.DeviceIdType.MESH
STREAMS = 2
PIECES = 2
TAIL_IN_SCATTER = (1, 1, 3, 6)
TAIL_IN_GATHER = (0, 0, 2, 5)
LANES = 128
BF16_ROWS = 16


def plain(tokens, up_weight, up_scale, down_weight, down_scale, pre_gain, post_gain):
    values = tokens.astype(jnp.float32)
    model_width = tokens.shape[1] * lax.axis_size("ra")
    stream = tokens
    for sublayer in range(up_weight.shape[0]):
        scaled = (values * pre_gain[sublayer][None, :]).astype(jnp.bfloat16)
        up_matrix = up_weight[sublayer].astype(jnp.bfloat16)
        down_matrix = down_weight[sublayer].astype(jnp.bfloat16)
        partial_up = jnp.dot(scaled, up_matrix, preferred_element_type=jnp.float32)
        whole_up = lax.psum(partial_up.astype(jnp.bfloat16), "ra").astype(jnp.float32)
        hidden = jnp.square(jax.nn.relu(whole_up * up_scale[sublayer][None, :])).astype(
            jnp.bfloat16
        )
        partial_down = jnp.dot(hidden, down_matrix, preferred_element_type=jnp.float32)
        summed = lax.psum(partial_down.astype(jnp.bfloat16), "cb").astype(jnp.float32)
        branch_in = summed * down_scale[sublayer][None, :]
        post_squares = lax.psum(jnp.sum(branch_in * branch_in, axis=1), "ra")
        inv_post = lax.rsqrt(post_squares / model_width + norm_eps)[:, None]
        branch = branch_in * inv_post * post_gain[sublayer][None, :]
        stream = (residual_keep * values + branch).astype(jnp.bfloat16)
        values = stream.astype(jnp.float32)
    return stream


def kernel(
    n, m, layers,
    tok_in, up, us_in, dn, ds_in, pg_in, qg_in,
    out,
    st_up, st_dn, wu, wd, xs, own, sendb, recvb, hid, acc, part_s, part_r, sums, ssq, ssall,
    tok, us, ds, pg, qg,
    w_sem, in_sem, rs_s, rs_r, ag_s, ag_r, pa_s, pa_r, su_s, su_r, ss_s, ss_r,
):
    f32, bf16 = jnp.float32, jnp.bfloat16
    ra, cb = lax.axis_index("ra"), lax.axis_index("cb")
    rows = xs.shape[1]
    dl = tok.shape[1]
    fc = wu.shape[2]
    fh = fc // 2
    sub = rows // PIECES
    far = n // 2

    def wrap(i):
        return lax.rem(i + 2 * n, n)

    half, odd = lax.div(ra, 2), lax.rem(ra, 2)
    p = half + odd * (n - 1 - 2 * half)

    def ra_of(q):
        hi = lax.div(q, n // 2)
        return 2 * q * (1 - hi) + hi * (2 * (n - 1 - q) + 1)

    target = [ra_of(wrap(p + 1)), ra_of(wrap(p - 1))]
    sign = [1, -1]
    long_flows = [(0, 0), (1, 1)]
    short_flows = [(0, 1), (1, 0)]
    flows = long_flows + short_flows

    def hops(d, e):
        return far if d == e else far - 1

    def chunk(q):
        return wrap(p + q)

    near_first = [0] + [q for k in range(1, far) for q in (k, -k)] + [far]
    far_first = near_first[::-1]

    def up_copy(l, i):
        c = chunk(far_first[i])
        return pltpu.make_async_copy(
            up.at[l, :, pl.ds(pl.multiple_of(c * fc, fc), fc)], st_up.at[i], w_sem.at[0, i]
        )

    def dn_copy(l, i):
        c = chunk(near_first[i])
        return pltpu.make_async_copy(
            dn.at[l, pl.ds(pl.multiple_of(c * fc, fc), fc), :], st_dn.at[i], w_sem.at[1, i]
        )

    def convert(src, dst, i, c):
        block = 32

        def body(j, _):
            r = pl.ds(pl.multiple_of(j * block, block), block)
            dst[c, r, :] = src[i, r, :].astype(bf16)
            return 0

        lax.fori_loop(0, src.shape[1] // block, body, 0)

    def take_up(l, chosen):
        for i in chosen:
            up_copy(l, i).wait()
            convert(st_up, wu, i, chunk(far_first[i]))
            if l + 1 < layers:
                up_copy(l + 1, i).start()

    def take_dn(l, chosen):
        for i in chosen:
            dn_copy(l, i).wait()
            convert(st_dn, wd, i, chunk(near_first[i]))
            if l + 1 < layers:
                dn_copy(l + 1, i).start()

    def part(h):
        return pl.ds(h * sub, sub)

    def rs_copy(l, g, d, e, j, h):
        return pltpu.make_async_remote_copy(
            src_ref=sendb.at[g, d, e, j, part(h), :],
            dst_ref=recvb.at[l, g, d, e, j, part(h), :],
            send_sem=rs_s.at[l, g, d, e, j, h], recv_sem=rs_r.at[l, g, d, e, j, h],
            device_id={"ra": target[d]}, device_id_type=MESH,
        )

    def ag_copy(l, g, d, e, s, h, arriving=False):
        c = chunk(-sign[d] * (s if arriving else s - 1))
        piece = hid.at[l, g, c, e, part(h), :]
        return pltpu.make_async_remote_copy(
            src_ref=piece, dst_ref=piece,
            send_sem=ag_s.at[l, g, d, e, s - 1, h], recv_sem=ag_r.at[l, g, d, e, s - 1, h],
            device_id={"ra": target[d]}, device_id_type=MESH,
        )

    def part_copy(l, g, k):
        return pltpu.make_async_remote_copy(
            src_ref=part_s.at[l, g, lax.rem(cb + k, m)], dst_ref=part_r.at[l, g, k - 1],
            send_sem=pa_s.at[l, g, k - 1], recv_sem=pa_r.at[l, g, k - 1],
            device_id={"cb": lax.rem(cb + k, m)}, device_id_type=MESH,
        )

    def sum_copy(l, g, k, who):
        return pltpu.make_async_remote_copy(
            src_ref=sums.at[l, g, who], dst_ref=sums.at[l, g, who],
            send_sem=su_s.at[l, g, k - 1], recv_sem=su_r.at[l, g, k - 1],
            device_id={"cb": lax.rem(cb + k, m)}, device_id_type=MESH,
        )

    def ss_copy(l, g, i, k, arriving=False):
        a, b = (lax.rem(ra + n - i, n), lax.rem(cb + m - k, m)) if arriving else (ra, cb)
        return pltpu.make_async_remote_copy(
            src_ref=ssall.at[l, g, b, a], dst_ref=ssall.at[l, g, b, a],
            send_sem=ss_s.at[l, g, i * m + k - 1], recv_sem=ss_r.at[l, g, i * m + k - 1],
            device_id={"ra": lax.rem(ra + i, n), "cb": lax.rem(cb + k, m)},
            device_id_type=MESH,
        )

    def dot(a, b):
        return jnp.dot(a, b, preferred_element_type=f32)

    def project(g, q):
        c = chunk(q)
        own[g, c] = dot(xs[g], wu[c])

    def mine(g, q, e, h):
        return own[g, chunk(q), h * sub : (h + 1) * sub, e * fh : (e + 1) * fh]

    def scatter(l, g, k, which):
        for h in range(PIECES):
            for d, e in which:
                j = k if d == e else k - 1
                v = mine(g, sign[d] * (far - k), e, h)
                if j > 0:
                    rs_copy(l, g, d, e, j - 1, h).wait_recv()
                    v = v + recvb[l, g, d, e, j - 1, part(h), :].astype(f32)
                sendb[g, d, e, j, part(h), :] = v.astype(bf16)
                rs_copy(l, g, d, e, j, h).start()

    def activate(l, g):
        project(g, 0)
        for e in (0, 1):
            scale = us[l : l + 1, pl.ds(pl.multiple_of(p * fc + e * fh, fh), fh)]
            for h in range(PIECES):
                v = mine(g, 0, e, h)
                for d in (0, 1):
                    j = hops(d, e) - 1
                    rs_copy(l, g, d, e, j, h).wait_recv()
                    v = v + recvb[l, g, d, e, j, part(h), :].astype(f32)
                v = jnp.maximum(v * scale, 0.0)
                hid[l, g, p, e, part(h), :] = (v * v).astype(bf16)

    def forward(l, g, s, which):
        for h in range(PIECES):
            for d, e in which:
                if s > 1:
                    ag_copy(l, g, d, e, s - 1, h, arriving=True).wait_recv()
                if s <= hops(d, e):
                    ag_copy(l, g, d, e, s, h).start()

    def reduce_hidden(l, g, q, first=False):
        c = chunk(q)
        a = dot(hid[l, g, c, 0], wd[c, :fh, :]) + dot(hid[l, g, c, 1], wd[c, fh:, :])
        if first:
            acc[g] = a
        else:
            acc[g] += a

    quarter = rows // m
    others = [(i, k) for i in range(n) for k in range(m) if i or k]

    def share_parts(l, g):
        for who in range(m):
            part_s[l, g, who] = acc[g, who * quarter : (who + 1) * quarter, :].astype(bf16)
        for k in range(1, m):
            part_copy(l, g, k).start()

    def share_sums(l, g):
        v = part_s[l, g, cb].astype(f32)
        for k in range(1, m):
            part_copy(l, g, k).wait_recv()
            v = v + part_r[l, g, k - 1].astype(f32)
        v = v.astype(bf16)
        sums[l, g, cb] = v
        for k in range(1, m):
            sum_copy(l, g, k, cb).start()
        b = v.astype(f32) * ds[l : l + 1, :]
        b = b * b
        t = b[:, :LANES]
        for j in range(1, dl // LANES):
            t = t + b[:, j * LANES : (j + 1) * LANES]
        ssq[:quarter, :] = t
        ssall[l, g, cb, ra] = jnp.sum(jnp.transpose(ssq[...]), axis=0, keepdims=True)
        for i, k in others:
            ss_copy(l, g, i, k).start()

    def renew(l, g):
        for k in range(1, m):
            sum_copy(l, g, k, lax.rem(cb + m - k, m)).wait_recv()
        for i, k in others:
            ss_copy(l, g, i, k, arriving=True).wait_recv()
        before = tok if l == 0 else out
        for who in range(m):
            t = ssall[l, g, who, 0]
            for i in range(1, n):
                t = t + ssall[l, g, who, i]
            t = lax.rsqrt(t / (dl * n) + norm_eps)
            inv = jnp.transpose(jnp.broadcast_to(t, (LANES, ssq.shape[0])))[:quarter, :]
            at = slice(g * rows + who * quarter, g * rows + (who + 1) * quarter)
            for j in range(dl // LANES):
                col = slice(j * LANES, (j + 1) * LANES)
                b = sums[l, g, who, :, col].astype(f32) * ds[l : l + 1, col]
                branch = b * inv * qg[l : l + 1, col]
                new = (residual_keep * before[at, col].astype(f32) + branch).astype(bf16)
                out[at, col] = new
                if l + 1 < layers:
                    xs[g, who * quarter : (who + 1) * quarter, col] = (
                        new.astype(f32) * pg[l + 1 : l + 2, col]
                    ).astype(bf16)

    def drain_scatter(l, g):
        for d, e in flows:
            for j in range(hops(d, e)):
                for h in range(PIECES):
                    rs_copy(l, g, d, e, j, h).wait_send()

    def drain_rest(l, g):
        for d, e in flows:
            for s in range(1, hops(d, e) + 1):
                for h in range(PIECES):
                    ag_copy(l, g, d, e, s, h).wait_send()
        for k in range(1, m):
            part_copy(l, g, k).wait_send()
            sum_copy(l, g, k, cb).wait_send()
        for i, k in others:
            ss_copy(l, g, i, k).wait_send()

    barrier = pltpu.get_barrier_semaphore()
    for d in (0, 1):
        pl.semaphore_signal(
            barrier, inc=1, device_id={"ra": target[d]}, device_id_type=MESH
        )
    for k in range(1, m):
        pl.semaphore_signal(
            barrier, inc=1, device_id={"cb": lax.rem(cb + k, m)}, device_id_type=MESH
        )

    inputs = [
        pltpu.make_async_copy(src, dst, in_sem.at[i])
        for i, (src, dst) in enumerate(
            [(pg_in, pg), (tok_in, tok), (us_in, us), (ds_in, ds), (qg_in, qg)]
        )
    ]
    for copy in inputs:
        copy.start()
    for i in range(n):
        up_copy(0, i).start()
    ssq[...] = jnp.zeros_like(ssq)
    for copy in inputs:
        copy.wait()
    for g in range(STREAMS):
        xs[g] = (tok[g * rows : (g + 1) * rows, :].astype(f32) * pg[0:1, :]).astype(bf16)

    def tail_steps(l, g):
        def end():
            forward(l, g, far + 1, long_flows)
            reduce_hidden(l, g, far)
            share_parts(l, g)

        def short_end():
            forward(l, g, far, short_flows)
            reduce_hidden(l, g, far - 1)
            reduce_hidden(l, g, 1 - far)

        return [
            short_end, end, lambda: share_sums(l, g), lambda: renew(l, g),
        ]

    def scatter_steps(l, g):
        fresh = l == 0 and g == 0

        def first():
            if fresh:
                take_up(l, [0])
            project(g, far)
            if fresh:
                pl.semaphore_wait(barrier, m + 1)
            scatter(l, g, 0, long_flows)

        def short(k):
            if fresh:
                take_up(l, [2 * k - 1, 2 * k])
                if k == 1:
                    for i in range(n):
                        dn_copy(l, i).start()
                if k == far - 1:
                    take_up(l, [n - 1])
            project(g, far - k)
            project(g, k - far)
            scatter(l, g, k, short_flows)

        steps = [first]
        for k in range(1, far):
            steps.append(functools.partial(short, k))
            steps.append(functools.partial(scatter, l, g, k, long_flows))
        return steps

    def gather_steps(l, g):
        def begin():
            forward(l, g, 1, long_flows)
            forward(l, g, 1, short_flows)
            reduce_hidden(l, g, 0, first=True)

        def short(s):
            forward(l, g, s, short_flows)
            reduce_hidden(l, g, s - 1)
            reduce_hidden(l, g, 1 - s)

        steps = [begin]
        for s in range(2, far + 1):
            steps.append(functools.partial(forward, l, g, s, long_flows))
            if s < far:
                steps.append(functools.partial(short, s))
        return steps

    def run(steps, side, slots):
        slots = [min(at, len(steps) - 1) for at in slots]
        for i, step in enumerate(steps):
            step()
            for extra, at in zip(side, slots):
                if at == i:
                    extra()

    pending, first_half, second_half = [], range(n // 2), range(n // 2, n)
    for l in range(layers):
        run(scatter_steps(l, 0), pending, TAIL_IN_SCATTER)
        run(
            scatter_steps(l, 1),
            [
                lambda: activate(l, 0), lambda: take_dn(l, first_half),
                lambda: take_dn(l, second_half),
            ],
            (1, 2, 3),
        )
        side = [lambda: activate(l, 1), lambda: drain_scatter(l, 0)]
        if l + 1 < layers:
            side += [
                lambda: take_up(l + 1, first_half), lambda: take_up(l + 1, second_half)
            ]
        run(gather_steps(l, 0), side, (0, 4, 2, 3))
        run(
            gather_steps(l, 1), tail_steps(l, 0) + [lambda: drain_scatter(l, 1)],
            TAIL_IN_GATHER + (4,),
        )
        pending = tail_steps(l, 1)
    for step in pending:
        step()
    for l in range(layers):
        for g in range(STREAMS):
            drain_rest(l, g)


def local(n, m, tokens, up_weight, up_scale, down_weight, down_scale, pre_gain, post_gain):
    t, dl = tokens.shape
    layers, _, fl = up_weight.shape
    fits = (
        n % 2 == 0 and n >= 4 and m >= 2 and t % (STREAMS * PIECES * BF16_ROWS) == 0
        and t % (STREAMS * m * BF16_ROWS) == 0 and fl % (2 * n * LANES) == 0
        and dl % LANES == 0
    )
    if not fits:
        return plain(
            tokens, up_weight, up_scale, down_weight, down_scale, pre_gain, post_gain
        )
    rows, fc, far = t // STREAMS, fl // n, n // 2
    lane_rows = -(-(rows // m) // LANES) * LANES
    f32, bf16 = jnp.float32, jnp.bfloat16
    vmem = pl.BlockSpec(memory_space=pltpu.VMEM)
    hbm = pl.BlockSpec(memory_space=pltpu.HBM)
    dma = pltpu.SemaphoreType.DMA
    return pl.pallas_call(
        functools.partial(kernel, n, m, layers),
        out_shape=pltpu.VMEM((t, dl), bf16),
        in_specs=[hbm] * 7,
        out_specs=vmem,
        scratch_shapes=[
            pltpu.VMEM((n, dl, fc), f32),
            pltpu.VMEM((n, fc, dl), f32),
            pltpu.VMEM((n, dl, fc), bf16),
            pltpu.VMEM((n, fc, dl), bf16),
            pltpu.VMEM((STREAMS, rows, dl), bf16),
            pltpu.VMEM((STREAMS, n, rows, fc), f32),
            pltpu.VMEM((STREAMS, 2, 2, far, rows, fc // 2), bf16),
            pltpu.VMEM((layers, STREAMS, 2, 2, far, rows, fc // 2), bf16),
            pltpu.VMEM((layers, STREAMS, n, 2, rows, fc // 2), bf16),
            pltpu.VMEM((STREAMS, rows, dl), f32),
            pltpu.VMEM((layers, STREAMS, m, rows // m, dl), bf16),
            pltpu.VMEM((layers, STREAMS, m - 1, rows // m, dl), bf16),
            pltpu.VMEM((layers, STREAMS, m, rows // m, dl), bf16),
            pltpu.VMEM((lane_rows, LANES), f32),
            pltpu.VMEM((layers, STREAMS, m, n, 1, lane_rows), f32),
            pltpu.VMEM((t, dl), bf16),
            pltpu.VMEM(up_scale.shape, f32),
            pltpu.VMEM(down_scale.shape, f32),
            pltpu.VMEM(pre_gain.shape, f32),
            pltpu.VMEM(post_gain.shape, f32),
            dma((2, n)),
            dma((5,)),
            dma((layers, STREAMS, 2, 2, far, PIECES)),
            dma((layers, STREAMS, 2, 2, far, PIECES)),
            dma((layers, STREAMS, 2, 2, far, PIECES)),
            dma((layers, STREAMS, 2, 2, far, PIECES)),
            dma((layers, STREAMS, m - 1)),
            dma((layers, STREAMS, m - 1)),
            dma((layers, STREAMS, m - 1)),
            dma((layers, STREAMS, m - 1)),
            dma((layers, STREAMS, n * m - 1)),
            dma((layers, STREAMS, n * m - 1)),
        ],
        compiler_params=pltpu.CompilerParams(
            collective_id=0, has_side_effects=True, vmem_limit_bytes=60 * 1024 * 1024
        ),
    )(tokens, up_weight, up_scale, down_weight, down_scale, pre_gain, post_gain)


def solution(mesh):
    return jax.shard_map(
        functools.partial(local, mesh.shape["ra"], mesh.shape["cb"]),
        mesh=mesh,
        in_specs=(
            P(None, "ra"),
            P(None, "ra", "cb"),
            P(None, "cb"),
            P(None, "cb", "ra"),
            P(None, "ra"),
            P(None, "ra"),
            P(None, "ra"),
        ),
        out_specs=P(None, "ra"),
        check_vma=False,
    )
```

```python
import functools

import jax
import jax.numpy as jnp
from jax import lax
from jax.experimental import pallas as pl
from jax.experimental.pallas import tpu as pltpu
from jax.sharding import PartitionSpec as P

norm_eps = 1e-06
residual_keep = 0.5
MESH = pl.DeviceIdType.MESH
STREAMS = 2
PIECES = 2
AHEAD = 2
TAIL_IN_SCATTER = (1, 1, 3, 6)
TAIL_IN_GATHER = (0, 0, 2, 5)
LANES = 128
BF16_ROWS = 16


def plain(tokens, up_weight, up_scale, down_weight, down_scale, pre_gain, post_gain):
    values = tokens.astype(jnp.float32)
    model_width = tokens.shape[1] * lax.axis_size("ra")
    stream = tokens
    for sublayer in range(up_weight.shape[0]):
        scaled = (values * pre_gain[sublayer][None, :]).astype(jnp.bfloat16)
        up_matrix = up_weight[sublayer].astype(jnp.bfloat16)
        down_matrix = down_weight[sublayer].astype(jnp.bfloat16)
        partial_up = jnp.dot(scaled, up_matrix, preferred_element_type=jnp.float32)
        whole_up = lax.psum(partial_up.astype(jnp.bfloat16), "ra").astype(jnp.float32)
        hidden = jnp.square(jax.nn.relu(whole_up * up_scale[sublayer][None, :])).astype(
            jnp.bfloat16
        )
        partial_down = jnp.dot(hidden, down_matrix, preferred_element_type=jnp.float32)
        summed = lax.psum(partial_down.astype(jnp.bfloat16), "cb").astype(jnp.float32)
        branch_in = summed * down_scale[sublayer][None, :]
        post_squares = lax.psum(jnp.sum(branch_in * branch_in, axis=1), "ra")
        inv_post = lax.rsqrt(post_squares / model_width + norm_eps)[:, None]
        branch = branch_in * inv_post * post_gain[sublayer][None, :]
        stream = (residual_keep * values + branch).astype(jnp.bfloat16)
        values = stream.astype(jnp.float32)
    return stream


def kernel(
    n, m, layers,
    tok_in, up, us_in, dn, ds_in, pg_in, qg_in,
    out,
    st_up, st_dn, wu, wd, xs, own, sendb, recvb, hid, acc, part_s, part_r, sums, ssq, ssall,
    tok, us, ds, pg, qg,
    w_sem, in_sem, rs_s, rs_r, ag_s, ag_r, pa_s, pa_r, su_s, su_r, ss_s, ss_r,
):
    f32, bf16 = jnp.float32, jnp.bfloat16
    ra, cb = lax.axis_index("ra"), lax.axis_index("cb")
    rows = xs.shape[1]
    dl = tok.shape[1]
    fc = wu.shape[2]
    fh = fc // 2
    sub = rows // PIECES
    far = n // 2

    def wrap(i):
        return lax.rem(i + 2 * n, n)

    half, odd = lax.div(ra, 2), lax.rem(ra, 2)
    p = half + odd * (n - 1 - 2 * half)

    def ra_of(q):
        hi = lax.div(q, n // 2)
        return 2 * q * (1 - hi) + hi * (2 * (n - 1 - q) + 1)

    target = [ra_of(wrap(p + 1)), ra_of(wrap(p - 1))]
    sign = [1, -1]
    long_flows = [(0, 0), (1, 1)]
    short_flows = [(0, 1), (1, 0)]
    flows = long_flows + short_flows

    def hops(d, e):
        return far if d == e else far - 1

    def chunk(q):
        return wrap(p + q)

    near_first = [0] + [q for k in range(1, far) for q in (k, -k)] + [far]
    far_first = near_first[::-1]

    def up_copy(l, i):
        c = chunk(far_first[i])
        return pltpu.make_async_copy(
            up.at[l, :, pl.ds(pl.multiple_of(c * fc, fc), fc)], st_up.at[i], w_sem.at[0, i]
        )

    def dn_copy(l, i):
        c = chunk(near_first[i])
        return pltpu.make_async_copy(
            dn.at[l, pl.ds(pl.multiple_of(c * fc, fc), fc), :], st_dn.at[i], w_sem.at[1, i]
        )

    def convert(src, dst, i, c):
        block = 32

        def body(j, _):
            r = pl.ds(pl.multiple_of(j * block, block), block)
            dst[c, r, :] = src[i, r, :].astype(bf16)
            return 0

        lax.fori_loop(0, src.shape[1] // block, body, 0)

    def take_up(l, chosen):
        for i in chosen:
            up_copy(l, i).wait()
            if l == 0 and i + AHEAD < n:
                up_copy(0, i + AHEAD).start()
            convert(st_up, wu, i, chunk(far_first[i]))
            if l + 1 < layers:
                up_copy(l + 1, i).start()

    def take_dn(l, chosen):
        for i in chosen:
            dn_copy(l, i).wait()
            convert(st_dn, wd, i, chunk(near_first[i]))
            if l + 1 < layers:
                dn_copy(l + 1, i).start()

    def part(h):
        return pl.ds(h * sub, sub)

    def rs_copy(l, g, d, e, j, h):
        return pltpu.make_async_remote_copy(
            src_ref=sendb.at[g, d, e, j, part(h), :],
            dst_ref=recvb.at[l, g, d, e, j, part(h), :],
            send_sem=rs_s.at[l, g, d, e, j, h], recv_sem=rs_r.at[l, g, d, e, j, h],
            device_id={"ra": target[d]}, device_id_type=MESH,
        )

    def ag_copy(l, g, d, e, s, h, arriving=False):
        c = chunk(-sign[d] * (s if arriving else s - 1))
        piece = hid.at[l, g, c, e, part(h), :]
        return pltpu.make_async_remote_copy(
            src_ref=piece, dst_ref=piece,
            send_sem=ag_s.at[l, g, d, e, s - 1, h], recv_sem=ag_r.at[l, g, d, e, s - 1, h],
            device_id={"ra": target[d]}, device_id_type=MESH,
        )

    def part_copy(l, g, k):
        return pltpu.make_async_remote_copy(
            src_ref=part_s.at[l, g, lax.rem(cb + k, m)], dst_ref=part_r.at[l, g, k - 1],
            send_sem=pa_s.at[l, g, k - 1], recv_sem=pa_r.at[l, g, k - 1],
            device_id={"cb": lax.rem(cb + k, m)}, device_id_type=MESH,
        )

    def sum_copy(l, g, k, who):
        return pltpu.make_async_remote_copy(
            src_ref=sums.at[l, g, who], dst_ref=sums.at[l, g, who],
            send_sem=su_s.at[l, g, k - 1], recv_sem=su_r.at[l, g, k - 1],
            device_id={"cb": lax.rem(cb + k, m)}, device_id_type=MESH,
        )

    def ss_copy(l, g, i, k, arriving=False):
        a, b = (lax.rem(ra + n - i, n), lax.rem(cb + m - k, m)) if arriving else (ra, cb)
        return pltpu.make_async_remote_copy(
            src_ref=ssall.at[l, g, b, a], dst_ref=ssall.at[l, g, b, a],
            send_sem=ss_s.at[l, g, i * m + k - 1], recv_sem=ss_r.at[l, g, i * m + k - 1],
            device_id={"ra": lax.rem(ra + i, n), "cb": lax.rem(cb + k, m)},
            device_id_type=MESH,
        )

    def dot(a, b):
        return jnp.dot(a, b, preferred_element_type=f32)

    def project(g, q):
        c = chunk(q)
        own[g, c] = dot(xs[g], wu[c])

    def mine(g, q, e, h):
        return own[g, chunk(q), h * sub : (h + 1) * sub, e * fh : (e + 1) * fh]

    def scatter(l, g, k, which):
        for h in range(PIECES):
            for d, e in which:
                j = k if d == e else k - 1
                v = mine(g, sign[d] * (far - k), e, h)
                if j > 0:
                    rs_copy(l, g, d, e, j - 1, h).wait_recv()
                    v = v + recvb[l, g, d, e, j - 1, part(h), :].astype(f32)
                sendb[g, d, e, j, part(h), :] = v.astype(bf16)
                rs_copy(l, g, d, e, j, h).start()

    def activate(l, g):
        project(g, 0)
        for e in (0, 1):
            scale = us[l : l + 1, pl.ds(pl.multiple_of(p * fc + e * fh, fh), fh)]
            for h in range(PIECES):
                v = mine(g, 0, e, h)
                for d in (0, 1):
                    j = hops(d, e) - 1
                    rs_copy(l, g, d, e, j, h).wait_recv()
                    v = v + recvb[l, g, d, e, j, part(h), :].astype(f32)
                v = jnp.maximum(v * scale, 0.0)
                hid[l, g, p, e, part(h), :] = (v * v).astype(bf16)

    def forward(l, g, s, which):
        for h in range(PIECES):
            for d, e in which:
                if s > 1:
                    ag_copy(l, g, d, e, s - 1, h, arriving=True).wait_recv()
                if s <= hops(d, e):
                    ag_copy(l, g, d, e, s, h).start()

    def reduce_hidden(l, g, q, first=False):
        c = chunk(q)
        a = dot(hid[l, g, c, 0], wd[c, :fh, :]) + dot(hid[l, g, c, 1], wd[c, fh:, :])
        if first:
            acc[g] = a
        else:
            acc[g] += a

    quarter = rows // m
    others = [(i, k) for i in range(n) for k in range(m) if i or k]

    def first_row(who):
        return (who % PIECES) * sub + who // PIECES * quarter

    def share_parts(l, g, h):
        c = chunk(far)
        a = dot(hid[l, g, c, 0, part(h), :], wd[c, :fh, :])
        a = a + dot(hid[l, g, c, 1, part(h), :], wd[c, fh:, :])
        a = (a + acc[g, part(h), :]).astype(bf16)
        for i in range(m // PIECES):
            part_s[l, g, i * PIECES + h] = a[i * quarter : (i + 1) * quarter, :]
        for k in range(1, m):
            @pl.when(lax.rem(cb + k, PIECES) == h)
            def _():
                part_copy(l, g, k).start()

    def share_sums(l, g):
        v = part_s[l, g, cb].astype(f32)
        for k in range(1, m):
            part_copy(l, g, k).wait_recv()
            v = v + part_r[l, g, k - 1].astype(f32)
        v = v.astype(bf16)
        sums[l, g, cb] = v
        for k in range(1, m):
            sum_copy(l, g, k, cb).start()
        b = v.astype(f32) * ds[l : l + 1, :]
        b = b * b
        t = b[:, :LANES]
        for j in range(1, dl // LANES):
            t = t + b[:, j * LANES : (j + 1) * LANES]
        ssq[:quarter, :] = t
        ssall[l, g, cb, ra] = jnp.sum(jnp.transpose(ssq[...]), axis=0, keepdims=True)
        for i, k in others:
            ss_copy(l, g, i, k).start()

    def renew(l, g):
        for k in range(1, m):
            sum_copy(l, g, k, lax.rem(cb + m - k, m)).wait_recv()
        for i, k in others:
            ss_copy(l, g, i, k, arriving=True).wait_recv()
        before = tok if l == 0 else out
        for who in range(m):
            t = ssall[l, g, who, 0]
            for i in range(1, n):
                t = t + ssall[l, g, who, i]
            t = lax.rsqrt(t / (dl * n) + norm_eps)
            inv = jnp.transpose(jnp.broadcast_to(t, (LANES, ssq.shape[0])))[:quarter, :]
            low = first_row(who)
            at = slice(g * rows + low, g * rows + low + quarter)
            for j in range(dl // LANES):
                col = slice(j * LANES, (j + 1) * LANES)
                b = sums[l, g, who, :, col].astype(f32) * ds[l : l + 1, col]
                branch = b * inv * qg[l : l + 1, col]
                new = (residual_keep * before[at, col].astype(f32) + branch).astype(bf16)
                out[at, col] = new
                if l + 1 < layers:
                    xs[g, low : low + quarter, col] = (
                        new.astype(f32) * pg[l + 1 : l + 2, col]
                    ).astype(bf16)

    def drain_scatter(l, g):
        for d, e in flows:
            for j in range(hops(d, e)):
                for h in range(PIECES):
                    rs_copy(l, g, d, e, j, h).wait_send()

    def drain_rest(l, g):
        for d, e in flows:
            for s in range(1, hops(d, e) + 1):
                for h in range(PIECES):
                    ag_copy(l, g, d, e, s, h).wait_send()
        for k in range(1, m):
            part_copy(l, g, k).wait_send()
            sum_copy(l, g, k, cb).wait_send()
        for i, k in others:
            ss_copy(l, g, i, k).wait_send()

    barrier = pltpu.get_barrier_semaphore()
    for d in (0, 1):
        pl.semaphore_signal(
            barrier, inc=1, device_id={"ra": target[d]}, device_id_type=MESH
        )
    for k in range(1, m):
        pl.semaphore_signal(
            barrier, inc=1, device_id={"cb": lax.rem(cb + k, m)}, device_id_type=MESH
        )

    inputs = [
        pltpu.make_async_copy(src, dst, in_sem.at[i])
        for i, (src, dst) in enumerate(
            [(pg_in, pg), (tok_in, tok), (us_in, us), (ds_in, ds), (qg_in, qg)]
        )
    ]
    for copy in inputs:
        copy.start()
    for i in range(AHEAD):
        up_copy(0, i).start()
    ssq[...] = jnp.zeros_like(ssq)
    for copy in inputs:
        copy.wait()
    for g in range(STREAMS):
        xs[g] = (tok[g * rows : (g + 1) * rows, :].astype(f32) * pg[0:1, :]).astype(bf16)

    def tail_steps(l, g):
        def end():
            for h in range(PIECES):
                for d, e in long_flows:
                    ag_copy(l, g, d, e, far, h, arriving=True).wait_recv()
                share_parts(l, g, h)

        def short_end():
            forward(l, g, far, short_flows)
            reduce_hidden(l, g, far - 1)
            reduce_hidden(l, g, 1 - far)

        def settle():
            drain_rest(l, g)
            renew(l, g)

        return [short_end, end, lambda: share_sums(l, g), settle]

    def scatter_steps(l, g):
        fresh = l == 0 and g == 0

        def first():
            if fresh:
                take_up(l, [0])
            project(g, far)
            if fresh:
                pl.semaphore_wait(barrier, m + 1)
            scatter(l, g, 0, long_flows)

        def short(k):
            if fresh:
                take_up(l, [2 * k - 1, 2 * k])
                if k == far - 1:
                    for i in range(n):
                        dn_copy(l, i).start()
                if k == far - 1:
                    take_up(l, [n - 1])
            project(g, far - k)
            project(g, k - far)
            scatter(l, g, k, short_flows)

        steps = [first]
        for k in range(1, far):
            steps.append(functools.partial(short, k))
            steps.append(functools.partial(scatter, l, g, k, long_flows))
        return steps

    def gather_steps(l, g):
        def begin():
            forward(l, g, 1, long_flows)
            forward(l, g, 1, short_flows)
            reduce_hidden(l, g, 0, first=True)

        def short(s):
            forward(l, g, s, short_flows)
            reduce_hidden(l, g, s - 1)
            reduce_hidden(l, g, 1 - s)

        steps = [begin]
        for s in range(2, far + 1):
            steps.append(functools.partial(forward, l, g, s, long_flows))
            if s < far:
                steps.append(functools.partial(short, s))
        return steps

    def run(steps, side, slots):
        slots = [min(at, len(steps) - 1) for at in slots]
        for i, step in enumerate(steps):
            step()
            for extra, at in zip(side, slots):
                if at == i:
                    extra()

    pending, first_half, second_half = [], range(n // 2), range(n // 2, n)
    for l in range(layers):
        run(scatter_steps(l, 0), pending, TAIL_IN_SCATTER)
        run(
            scatter_steps(l, 1),
            [
                lambda: activate(l, 0), lambda: take_dn(l, first_half),
                lambda: take_dn(l, second_half),
            ],
            (1, 2, 3),
        )
        side = [lambda: activate(l, 1), lambda: drain_scatter(l, 0)]
        if l + 1 < layers:
            side += [
                lambda: take_up(l + 1, first_half), lambda: take_up(l + 1, second_half)
            ]
        run(gather_steps(l, 0), side, (0, 4, 2, 3))
        run(
            gather_steps(l, 1), tail_steps(l, 0) + [lambda: drain_scatter(l, 1)],
            TAIL_IN_GATHER + (4,),
        )
        pending = tail_steps(l, 1)
    for step in pending:
        step()


def local(n, m, tokens, up_weight, up_scale, down_weight, down_scale, pre_gain, post_gain):
    t, dl = tokens.shape
    layers, _, fl = up_weight.shape
    fits = (
        n % 2 == 0 and n >= 4 and m >= 2 and t % (STREAMS * PIECES * BF16_ROWS) == 0
        and m % PIECES == 0 and t % (STREAMS * m * BF16_ROWS) == 0 and fl % (2 * n * LANES) == 0
        and dl % LANES == 0
    )
    if not fits:
        return plain(
            tokens, up_weight, up_scale, down_weight, down_scale, pre_gain, post_gain
        )
    rows, fc, far = t // STREAMS, fl // n, n // 2
    lane_rows = -(-(rows // m) // LANES) * LANES
    f32, bf16 = jnp.float32, jnp.bfloat16
    vmem = pl.BlockSpec(memory_space=pltpu.VMEM)
    hbm = pl.BlockSpec(memory_space=pltpu.HBM)
    dma = pltpu.SemaphoreType.DMA
    return pl.pallas_call(
        functools.partial(kernel, n, m, layers),
        out_shape=pltpu.VMEM((t, dl), bf16),
        in_specs=[hbm] * 7,
        out_specs=vmem,
        scratch_shapes=[
            pltpu.VMEM((n, dl, fc), f32),
            pltpu.VMEM((n, fc, dl), f32),
            pltpu.VMEM((n, dl, fc), bf16),
            pltpu.VMEM((n, fc, dl), bf16),
            pltpu.VMEM((STREAMS, rows, dl), bf16),
            pltpu.VMEM((STREAMS, n, rows, fc), f32),
            pltpu.VMEM((STREAMS, 2, 2, far, rows, fc // 2), bf16),
            pltpu.VMEM((layers, STREAMS, 2, 2, far, rows, fc // 2), bf16),
            pltpu.VMEM((layers, STREAMS, n, 2, rows, fc // 2), bf16),
            pltpu.VMEM((STREAMS, rows, dl), f32),
            pltpu.VMEM((layers, STREAMS, m, rows // m, dl), bf16),
            pltpu.VMEM((layers, STREAMS, m - 1, rows // m, dl), bf16),
            pltpu.VMEM((layers, STREAMS, m, rows // m, dl), bf16),
            pltpu.VMEM((lane_rows, LANES), f32),
            pltpu.VMEM((layers, STREAMS, m, n, 1, lane_rows), f32),
            pltpu.VMEM((t, dl), bf16),
            pltpu.VMEM(up_scale.shape, f32),
            pltpu.VMEM(down_scale.shape, f32),
            pltpu.VMEM(pre_gain.shape, f32),
            pltpu.VMEM(post_gain.shape, f32),
            dma((2, n)),
            dma((5,)),
            dma((layers, STREAMS, 2, 2, far, PIECES)),
            dma((layers, STREAMS, 2, 2, far, PIECES)),
            dma((layers, STREAMS, 2, 2, far, PIECES)),
            dma((layers, STREAMS, 2, 2, far, PIECES)),
            dma((layers, STREAMS, m - 1)),
            dma((layers, STREAMS, m - 1)),
            dma((layers, STREAMS, m - 1)),
            dma((layers, STREAMS, m - 1)),
            dma((layers, STREAMS, n * m - 1)),
            dma((layers, STREAMS, n * m - 1)),
        ],
        compiler_params=pltpu.CompilerParams(
            collective_id=0, has_side_effects=True, vmem_limit_bytes=60 * 1024 * 1024
        ),
    )(tokens, up_weight, up_scale, down_weight, down_scale, pre_gain, post_gain)


def solution(mesh):
    return jax.shard_map(
        functools.partial(local, mesh.shape["ra"], mesh.shape["cb"]),
        mesh=mesh,
        in_specs=(
            P(None, "ra"),
            P(None, "ra", "cb"),
            P(None, "cb"),
            P(None, "cb", "ra"),
            P(None, "ra"),
            P(None, "ra"),
            P(None, "ra"),
        ),
        out_specs=P(None, "ra"),
        check_vma=False,
    )
```

```python
import functools

import jax
import jax.numpy as jnp
from jax import lax
from jax.experimental import pallas as pl
from jax.experimental.pallas import tpu as pltpu
from jax.sharding import PartitionSpec as P

norm_eps = 1e-06
residual_keep = 0.5
MESH = pl.DeviceIdType.MESH
STREAMS = 2
PIECES = 2
AHEAD = 2
TAIL_IN_SCATTER = (1, 1, 3, 6)
TAIL_IN_GATHER = (0, 0, 2, 5)
LANES = 128
BF16_ROWS = 16


def plain(tokens, up_weight, up_scale, down_weight, down_scale, pre_gain, post_gain):
    values = tokens.astype(jnp.float32)
    model_width = tokens.shape[1] * lax.axis_size("ra")
    stream = tokens
    for sublayer in range(up_weight.shape[0]):
        scaled = (values * pre_gain[sublayer][None, :]).astype(jnp.bfloat16)
        up_matrix = up_weight[sublayer].astype(jnp.bfloat16)
        down_matrix = down_weight[sublayer].astype(jnp.bfloat16)
        partial_up = jnp.dot(scaled, up_matrix, preferred_element_type=jnp.float32)
        whole_up = lax.psum(partial_up.astype(jnp.bfloat16), "ra").astype(jnp.float32)
        hidden = jnp.square(jax.nn.relu(whole_up * up_scale[sublayer][None, :])).astype(
            jnp.bfloat16
        )
        partial_down = jnp.dot(hidden, down_matrix, preferred_element_type=jnp.float32)
        summed = lax.psum(partial_down.astype(jnp.bfloat16), "cb").astype(jnp.float32)
        branch_in = summed * down_scale[sublayer][None, :]
        post_squares = lax.psum(jnp.sum(branch_in * branch_in, axis=1), "ra")
        inv_post = lax.rsqrt(post_squares / model_width + norm_eps)[:, None]
        branch = branch_in * inv_post * post_gain[sublayer][None, :]
        stream = (residual_keep * values + branch).astype(jnp.bfloat16)
        values = stream.astype(jnp.float32)
    return stream


def kernel(
    n, m, layers,
    tok_in, up, us_in, dn, ds_in, pg_in, qg_in,
    out,
    st_up, st_dn, wu, wd, xs, own, sendb, recvb, hid, acc, part_s, part_r, sums, ssq, ssall,
    tok, us, ds, pg, qg,
    w_sem, in_sem, rs_s, rs_r, ag_s, ag_r, pa_s, pa_r, su_s, su_r, ss_s, ss_r,
):
    f32, bf16 = jnp.float32, jnp.bfloat16
    ra, cb = lax.axis_index("ra"), lax.axis_index("cb")
    rows = xs.shape[1]
    dl = tok.shape[1]
    fc = wu.shape[2]
    fh = fc // 2
    sub = rows // PIECES
    far = n // 2

    def wrap(i):
        return lax.rem(i + 2 * n, n)

    half, odd = lax.div(ra, 2), lax.rem(ra, 2)
    p = half + odd * (n - 1 - 2 * half)

    def ra_of(q):
        hi = lax.div(q, n // 2)
        return 2 * q * (1 - hi) + hi * (2 * (n - 1 - q) + 1)

    target = [ra_of(wrap(p + 1)), ra_of(wrap(p - 1))]
    sign = [1, -1]
    long_flows = [(0, 0), (1, 1)]
    short_flows = [(0, 1), (1, 0)]
    flows = long_flows + short_flows

    def hops(d, e):
        return far if d == e else far - 1

    def chunk(q):
        return wrap(p + q)

    near_first = [0] + [q for k in range(1, far) for q in (k, -k)] + [far]
    far_first = near_first[::-1]

    def up_copy(l, i):
        c = chunk(far_first[i])
        return pltpu.make_async_copy(
            up.at[l, :, pl.ds(pl.multiple_of(c * fc, fc), fc)], st_up.at[i], w_sem.at[0, i]
        )

    def dn_copy(l, i):
        c = chunk(near_first[i])
        return pltpu.make_async_copy(
            dn.at[l, pl.ds(pl.multiple_of(c * fc, fc), fc), :], st_dn.at[i], w_sem.at[1, i]
        )

    def convert(src, dst, i, c):
        block = 32

        def body(j, _):
            r = pl.ds(pl.multiple_of(j * block, block), block)
            dst[c, r, :] = src[i, r, :].astype(bf16)
            return 0

        lax.fori_loop(0, src.shape[1] // block, body, 0)

    def take_up(l, chosen):
        for i in chosen:
            up_copy(l, i).wait()
            if l == 0 and i + AHEAD < n:
                up_copy(0, i + AHEAD).start()
            convert(st_up, wu, i, chunk(far_first[i]))
            if l + 1 < layers:
                up_copy(l + 1, i).start()

    def take_dn(l, chosen):
        for i in chosen:
            dn_copy(l, i).wait()
            convert(st_dn, wd, i, chunk(near_first[i]))
            if l + 1 < layers:
                dn_copy(l + 1, i).start()

    def part(h):
        return pl.ds(h * sub, sub)

    def rs_copy(l, g, d, e, j, h):
        return pltpu.make_async_remote_copy(
            src_ref=sendb.at[g, d, e, j, part(h), :],
            dst_ref=recvb.at[l, g, d, e, j, part(h), :],
            send_sem=rs_s.at[l, g, d, e, j, h], recv_sem=rs_r.at[l, g, d, e, j, h],
            device_id={"ra": target[d]}, device_id_type=MESH,
        )

    def ag_copy(l, g, d, e, s, h, arriving=False):
        c = chunk(-sign[d] * (s if arriving else s - 1))
        piece = hid.at[l, g, c, e, part(h), :]
        return pltpu.make_async_remote_copy(
            src_ref=piece, dst_ref=piece,
            send_sem=ag_s.at[l, g, d, e, s - 1, h], recv_sem=ag_r.at[l, g, d, e, s - 1, h],
            device_id={"ra": target[d]}, device_id_type=MESH,
        )

    def part_copy(l, g, k):
        return pltpu.make_async_remote_copy(
            src_ref=part_s.at[l, g, lax.rem(cb + k, m)], dst_ref=part_r.at[l, g, k - 1],
            send_sem=pa_s.at[l, g, k - 1], recv_sem=pa_r.at[l, g, k - 1],
            device_id={"cb": lax.rem(cb + k, m)}, device_id_type=MESH,
        )

    def sum_copy(l, g, k, who):
        return pltpu.make_async_remote_copy(
            src_ref=sums.at[l, g, who], dst_ref=sums.at[l, g, who],
            send_sem=su_s.at[l, g, k - 1], recv_sem=su_r.at[l, g, k - 1],
            device_id={"cb": lax.rem(cb + k, m)}, device_id_type=MESH,
        )

    def ss_copy(l, g, i, k, arriving=False):
        a, b = (lax.rem(ra + n - i, n), lax.rem(cb + m - k, m)) if arriving else (ra, cb)
        return pltpu.make_async_remote_copy(
            src_ref=ssall.at[l, g, b, a], dst_ref=ssall.at[l, g, b, a],
            send_sem=ss_s.at[l, g, i * m + k - 1], recv_sem=ss_r.at[l, g, i * m + k - 1],
            device_id={"ra": lax.rem(ra + i, n), "cb": lax.rem(cb + k, m)},
            device_id_type=MESH,
        )

    def dot(a, b):
        return jnp.dot(a, b, preferred_element_type=f32)

    def project(g, q):
        c = chunk(q)
        own[g, c] = dot(xs[g], wu[c])

    def mine(g, q, e, h):
        return own[g, chunk(q), h * sub : (h + 1) * sub, e * fh : (e + 1) * fh]

    def scatter(l, g, k, which):
        for h in range(PIECES):
            for d, e in which:
                j = k if d == e else k - 1
                v = mine(g, sign[d] * (far - k), e, h)
                if j > 0:
                    rs_copy(l, g, d, e, j - 1, h).wait_recv()
                    v = v + recvb[l, g, d, e, j - 1, part(h), :].astype(f32)
                sendb[g, d, e, j, part(h), :] = v.astype(bf16)
                rs_copy(l, g, d, e, j, h).start()

    def activate(l, g):
        project(g, 0)
        for e in (0, 1):
            scale = us[l : l + 1, pl.ds(pl.multiple_of(p * fc + e * fh, fh), fh)]
            for h in range(PIECES):
                v = mine(g, 0, e, h)
                for d in (0, 1):
                    j = hops(d, e) - 1
                    rs_copy(l, g, d, e, j, h).wait_recv()
                    v = v + recvb[l, g, d, e, j, part(h), :].astype(f32)
                v = jnp.maximum(v * scale, 0.0)
                hid[l, g, p, e, part(h), :] = (v * v).astype(bf16)

    def forward(l, g, s, which):
        for h in range(PIECES):
            for d, e in which:
                if s > 1:
                    ag_copy(l, g, d, e, s - 1, h, arriving=True).wait_recv()
                if s <= hops(d, e):
                    ag_copy(l, g, d, e, s, h).start()

    def reduce_hidden(l, g, q, first=False):
        c = chunk(q)
        a = dot(hid[l, g, c, 0], wd[c, :fh, :]) + dot(hid[l, g, c, 1], wd[c, fh:, :])
        if first:
            acc[g] = a
        else:
            acc[g] += a

    quarter = rows // m
    others = [(i, k) for i in range(n) for k in range(m) if i or k]

    def first_row(who):
        return (who % PIECES) * sub + who // PIECES * quarter

    def share_parts(l, g, h):
        c = chunk(far)
        a = dot(hid[l, g, c, 0, part(h), :], wd[c, :fh, :])
        a = a + dot(hid[l, g, c, 1, part(h), :], wd[c, fh:, :])
        a = (a + acc[g, part(h), :]).astype(bf16)
        for i in range(m // PIECES):
            part_s[l, g, i * PIECES + h] = a[i * quarter : (i + 1) * quarter, :]
        for k in range(1, m):
            @pl.when(lax.rem(cb + k, PIECES) == h)
            def _():
                part_copy(l, g, k).start()

    def share_sums(l, g):
        v = part_s[l, g, cb].astype(f32)
        for k in range(1, m):
            part_copy(l, g, k).wait_recv()
            v = v + part_r[l, g, k - 1].astype(f32)
        v = v.astype(bf16)
        sums[l, g, cb] = v
        for k in range(1, m):
            sum_copy(l, g, k, cb).start()
        b = v.astype(f32) * ds[l : l + 1, :]
        b = b * b
        t = b[:, :LANES]
        for j in range(1, dl // LANES):
            t = t + b[:, j * LANES : (j + 1) * LANES]
        ssq[:quarter, :] = t
        ssall[l, g, cb, ra] = jnp.sum(jnp.transpose(ssq[...]), axis=0, keepdims=True)
        for i, k in others:
            ss_copy(l, g, i, k).start()

    def renew(l, g):
        for k in range(1, m):
            sum_copy(l, g, k, lax.rem(cb + m - k, m)).wait_recv()
        for i, k in others:
            ss_copy(l, g, i, k, arriving=True).wait_recv()
        before = tok if l == 0 else out
        for who in range(m):
            t = ssall[l, g, who, 0]
            for i in range(1, n):
                t = t + ssall[l, g, who, i]
            t = lax.rsqrt(t / (dl * n) + norm_eps)
            inv = jnp.transpose(jnp.broadcast_to(t, (LANES, ssq.shape[0])))[:quarter, :]
            low = first_row(who)
            at = slice(g * rows + low, g * rows + low + quarter)
            for j in range(dl // LANES):
                col = slice(j * LANES, (j + 1) * LANES)
                b = sums[l, g, who, :, col].astype(f32) * ds[l : l + 1, col]
                branch = b * inv * qg[l : l + 1, col]
                new = (residual_keep * before[at, col].astype(f32) + branch).astype(bf16)
                out[at, col] = new
                if l + 1 < layers:
                    xs[g, low : low + quarter, col] = (
                        new.astype(f32) * pg[l + 1 : l + 2, col]
                    ).astype(bf16)

    def drain_scatter(l, g):
        for d, e in flows:
            for j in range(hops(d, e)):
                for h in range(PIECES):
                    rs_copy(l, g, d, e, j, h).wait_send()

    def drain_rest(l, g):
        for d, e in flows:
            for s in range(1, hops(d, e) + 1):
                for h in range(PIECES):
                    ag_copy(l, g, d, e, s, h).wait_send()
        for k in range(1, m):
            part_copy(l, g, k).wait_send()
            sum_copy(l, g, k, cb).wait_send()
        for i, k in others:
            ss_copy(l, g, i, k).wait_send()

    barrier = pltpu.get_barrier_semaphore()
    for d in (0, 1):
        pl.semaphore_signal(
            barrier, inc=1, device_id={"ra": target[d]}, device_id_type=MESH
        )
    for k in range(1, m):
        pl.semaphore_signal(
            barrier, inc=1, device_id={"cb": lax.rem(cb + k, m)}, device_id_type=MESH
        )

    inputs = [
        pltpu.make_async_copy(src, dst, in_sem.at[i])
        for i, (src, dst) in enumerate(
            [(pg_in, pg), (tok_in, tok), (us_in, us), (ds_in, ds), (qg_in, qg)]
        )
    ]
    for copy in inputs[:2]:
        copy.start()
    for i in range(AHEAD):
        up_copy(0, i).start()
    for copy in inputs[2:]:
        copy.start()
    ssq[...] = jnp.zeros_like(ssq)
    for copy in inputs[:2]:
        copy.wait()

    def scale_in(g):
        xs[g] = (tok[g * rows : (g + 1) * rows, :].astype(f32) * pg[0:1, :]).astype(bf16)

    scale_in(0)

    def tail_steps(l, g):
        def end():
            for h in range(PIECES):
                for d, e in long_flows:
                    ag_copy(l, g, d, e, far, h, arriving=True).wait_recv()
                share_parts(l, g, h)

        def short_end():
            forward(l, g, far, short_flows)
            reduce_hidden(l, g, far - 1)
            reduce_hidden(l, g, 1 - far)

        def settle():
            drain_rest(l, g)
            renew(l, g)

        return [short_end, end, lambda: share_sums(l, g), settle]

    def scatter_steps(l, g):
        fresh = l == 0 and g == 0

        def first():
            if fresh:
                take_up(l, [0])
            project(g, far)
            if fresh:
                pl.semaphore_wait(barrier, m + 1)
            scatter(l, g, 0, long_flows)
            if fresh:
                for later in range(1, STREAMS):
                    scale_in(later)
                for copy in inputs[2:]:
                    copy.wait()

        def short(k):
            if fresh:
                take_up(l, [2 * k - 1, 2 * k])
                if k == far - 1:
                    for i in range(n):
                        dn_copy(l, i).start()
                if k == far - 1:
                    take_up(l, [n - 1])
            project(g, far - k)
            project(g, k - far)
            scatter(l, g, k, short_flows)

        steps = [first]
        for k in range(1, far):
            steps.append(functools.partial(short, k))
            steps.append(functools.partial(scatter, l, g, k, long_flows))
        return steps

    def gather_steps(l, g):
        def begin():
            forward(l, g, 1, long_flows)
            forward(l, g, 1, short_flows)
            reduce_hidden(l, g, 0, first=True)

        def short(s):
            forward(l, g, s, short_flows)
            reduce_hidden(l, g, s - 1)
            reduce_hidden(l, g, 1 - s)

        steps = [begin]
        for s in range(2, far + 1):
            steps.append(functools.partial(forward, l, g, s, long_flows))
            if s < far:
                steps.append(functools.partial(short, s))
        return steps

    def run(steps, side, slots):
        slots = [min(at, len(steps) - 1) for at in slots]
        for i, step in enumerate(steps):
            step()
            for extra, at in zip(side, slots):
                if at == i:
                    extra()

    pending, first_half, second_half = [], range(n // 2), range(n // 2, n)
    for l in range(layers):
        run(scatter_steps(l, 0), pending, TAIL_IN_SCATTER)
        run(
            scatter_steps(l, 1),
            [
                lambda: activate(l, 0), lambda: take_dn(l, first_half),
                lambda: take_dn(l, second_half),
            ],
            (1, 2, 3),
        )
        side = [lambda: activate(l, 1), lambda: drain_scatter(l, 0)]
        if l + 1 < layers:
            side += [
                lambda: take_up(l + 1, first_half), lambda: take_up(l + 1, second_half)
            ]
        run(gather_steps(l, 0), side, (0, 4, 2, 3))
        run(
            gather_steps(l, 1), tail_steps(l, 0) + [lambda: drain_scatter(l, 1)],
            TAIL_IN_GATHER + (4,),
        )
        pending = tail_steps(l, 1)
    for step in pending:
        step()


def local(n, m, tokens, up_weight, up_scale, down_weight, down_scale, pre_gain, post_gain):
    t, dl = tokens.shape
    layers, _, fl = up_weight.shape
    fits = (
        n % 2 == 0 and n >= 4 and m >= 2 and t % (STREAMS * PIECES * BF16_ROWS) == 0
        and m % PIECES == 0 and t % (STREAMS * m * BF16_ROWS) == 0 and fl % (2 * n * LANES) == 0
        and dl % LANES == 0
    )
    if not fits:
        return plain(
            tokens, up_weight, up_scale, down_weight, down_scale, pre_gain, post_gain
        )
    rows, fc, far = t // STREAMS, fl // n, n // 2
    lane_rows = -(-(rows // m) // LANES) * LANES
    f32, bf16 = jnp.float32, jnp.bfloat16
    vmem = pl.BlockSpec(memory_space=pltpu.VMEM)
    hbm = pl.BlockSpec(memory_space=pltpu.HBM)
    dma = pltpu.SemaphoreType.DMA
    return pl.pallas_call(
        functools.partial(kernel, n, m, layers),
        out_shape=pltpu.VMEM((t, dl), bf16),
        in_specs=[hbm] * 7,
        out_specs=vmem,
        scratch_shapes=[
            pltpu.VMEM((n, dl, fc), f32),
            pltpu.VMEM((n, fc, dl), f32),
            pltpu.VMEM((n, dl, fc), bf16),
            pltpu.VMEM((n, fc, dl), bf16),
            pltpu.VMEM((STREAMS, rows, dl), bf16),
            pltpu.VMEM((STREAMS, n, rows, fc), f32),
            pltpu.VMEM((STREAMS, 2, 2, far, rows, fc // 2), bf16),
            pltpu.VMEM((layers, STREAMS, 2, 2, far, rows, fc // 2), bf16),
            pltpu.VMEM((layers, STREAMS, n, 2, rows, fc // 2), bf16),
            pltpu.VMEM((STREAMS, rows, dl), f32),
            pltpu.VMEM((layers, STREAMS, m, rows // m, dl), bf16),
            pltpu.VMEM((layers, STREAMS, m - 1, rows // m, dl), bf16),
            pltpu.VMEM((layers, STREAMS, m, rows // m, dl), bf16),
            pltpu.VMEM((lane_rows, LANES), f32),
            pltpu.VMEM((layers, STREAMS, m, n, 1, lane_rows), f32),
            pltpu.VMEM((t, dl), bf16),
            pltpu.VMEM(up_scale.shape, f32),
            pltpu.VMEM(down_scale.shape, f32),
            pltpu.VMEM(pre_gain.shape, f32),
            pltpu.VMEM(post_gain.shape, f32),
            dma((2, n)),
            dma((5,)),
            dma((layers, STREAMS, 2, 2, far, PIECES)),
            dma((layers, STREAMS, 2, 2, far, PIECES)),
            dma((layers, STREAMS, 2, 2, far, PIECES)),
            dma((layers, STREAMS, 2, 2, far, PIECES)),
            dma((layers, STREAMS, m - 1)),
            dma((layers, STREAMS, m - 1)),
            dma((layers, STREAMS, m - 1)),
            dma((layers, STREAMS, m - 1)),
            dma((layers, STREAMS, n * m - 1)),
            dma((layers, STREAMS, n * m - 1)),
        ],
        compiler_params=pltpu.CompilerParams(
            collective_id=0, has_side_effects=True, vmem_limit_bytes=60 * 1024 * 1024
        ),
    )(tokens, up_weight, up_scale, down_weight, down_scale, pre_gain, post_gain)


def solution(mesh):
    return jax.shard_map(
        functools.partial(local, mesh.shape["ra"], mesh.shape["cb"]),
        mesh=mesh,
        in_specs=(
            P(None, "ra"),
            P(None, "ra", "cb"),
            P(None, "cb"),
            P(None, "cb", "ra"),
            P(None, "ra"),
            P(None, "ra"),
            P(None, "ra"),
        ),
        out_specs=P(None, "ra"),
        check_vma=False,
    )
```
